32 devices in a mesh: sp: 8 (over z, y), tp: 4 (over x, core).
Axes of the slice: x: 2, y: 2, z: 4, core: 2. Of those that a mesh axis runs over, the one named last changes fastest.
Arguments:
- hidden: bfloat16 [2048, 2048], P('sp'), may hold values from -6 to 6
- cotangent: bfloat16 [2048, 2048], P('sp'), may hold values from -6 to 6
- retained: bfloat16 [2048, 2048], P('sp', 'tp'), may hold values from -6 to 6
- queries: bfloat16 [2048, 1024], P('sp', 'tp'), may hold values from -1.5 to 1.5
- key_rows: bfloat16 [2048, 1024], P('sp', 'tp'), may hold values from -1.5 to 1.5
- value_rows: bfloat16 [2048, 2048], P('sp', 'tp'), may hold values from -0.25 to 0.25
- routes: int32 [2048, 2], P('sp'), may hold values from 0 to 7, all different within a row; in each aligned block of 256 rows (0 to 255, 256 to 511, ...) at most 96 rows name the same one
- route_weight: float32 [2048, 2], P('sp'), may hold values from 0.2 to 1.5
- gate_weight: bfloat16 [8, 2048, 1024], P('sp', None, 'tp'), may hold values from -0.125 to 0.125
- up_weight: bfloat16 [8, 2048, 1024], P('sp', None, 'tp'), may hold values from -0.125 to 0.125
- down_weight: bfloat16 [8, 1024, 2048], P('sp', 'tp'), may hold values from -0.1875 to 0.1875
- out_weight: bfloat16 [2048, 2048], P(None, 'tp'), may hold values from -0.125 to 0.125
Outputs:
- gate_grad: float32 [8, 2048, 1024], P('sp', None, 'tp')
- up_grad: float32 [8, 2048, 1024], P('sp', None, 'tp')
- down_grad: float32 [8, 1024, 2048], P('sp', 'tp')
- proj_grad: float32 [2048, 2048], P('sp', 'tp')
- query_gradient: float32 [2048, 1024], P('sp', 'tp')
- key_gradient: float32 [2048, 1024], P('sp', 'tp')
- value_gradient: float32 [2048, 2048], P('sp', 'tp')
The draws below stay inside these ranges and needn't reach their ends.
Inputs may be any that keep to these rules, and one draw needn't show every extreme that they name: `routes`: each row names 2 different experts; among the 256 rows of one index of sp no expert is named more than 96 times, a bound that some block reaches.
All inputs are finite; a program needn't handle non-finite values.
Results may differ from the reference program's by a relative error of at most 0.013.
Values may be sent and summed in bfloat16 or wider, within the bound.
A program may use at most 128 MiB of HBM per device.

```python
import math
import jax
import jax.numpy as jnp
import numpy as np
from jax import lax

D = 2048
H = 4
DK = 256
DV = 512
FF = 1024
TOP = 2
TOK_DEV = 256
TOKENS = 2048
EXPERTS = 8
CAP = 96
VW = 2048
N_SP = 8
N_TP = 4


def with_spikes(array, own_key, source, target, blocks, factor):
    owner, partner = [(jnp.arange(array.shape[position]) // (array.shape[position] // blocks)).reshape([-1 if axis == position else 1 for axis in range(array.ndim)]) for position in (source, target)]
    chosen = jax.random.permutation(own_key, blocks)[partner]
    strong = (owner == chosen) | (owner == (partner + blocks // 2) % blocks)
    return jnp.where(strong, factor * array, array)


def block_scale(own_key, shape, cuts, smallest, largest):
    level = 1.0
    for position, blocks in cuts:
        heights = jax.random.uniform(jax.random.fold_in(jax.random.fold_in(own_key, 6), position), (blocks,), jnp.float32, smallest / len(cuts), largest / len(cuts))
        level = level * jnp.repeat(jnp.exp(heights), shape[position] // blocks).reshape((-1,) + (1,) * (len(shape) - 1 - position))
    return level


def assign_block(key, own, number, rows, number_of, top, most, skew):
    sequence = jax.random.permutation(key, number_of)
    heavy_load, ordinary = portions_of(number_of, rows * top, most, skew, True), portions_of(number_of, rows * top, most, skew, False)
    places = jnp.arange(number_of)

    def named(tallies, offset_by):
        used = int((tallies > 0).sum())
        fixed = max(1, used // 4)
        passed = fixed + (places - fixed + offset_by * (used - fixed)) % max(1, number_of - fixed)
        return jnp.zeros((number_of,), jnp.int32).at[sequence[jnp.where(places < fixed, places, passed)]].set(jnp.asarray(tallies, jnp.int32))

    tallies = jnp.where(number % 4 == 0, named(heavy_load, number // 4), named(ordinary, number - number // 4 - 1))
    mixed = jax.random.permutation(jax.random.fold_in(own, 3), number_of)
    source_of, receiver = mixed[0:number_of // 2 * 2:2], mixed[1:number_of // 2 * 2:2]
    slack = jnp.minimum(tallies[source_of] - 1, most - tallies[receiver]) // 2
    slack = jnp.where((source_of == sequence[0]) | (receiver == sequence[0]) | (tallies[receiver] == 0), 0, jnp.maximum(slack, 0))
    passed = jax.random.randint(jax.random.fold_in(own, 4), (number_of // 2,), 0, 1 << 20) % (slack + 1)
    tallies = tallies.at[source_of].add(-passed).at[receiver].add(passed)
    members = jnp.searchsorted(jnp.cumsum(tallies), jnp.arange(rows * top), side="right").astype(jnp.int32)
    listing = members.reshape(top, rows).T
    listing = listing[jax.random.permutation(jax.random.fold_in(own, 1), rows)]
    offset_by = jax.random.randint(jax.random.fold_in(own, 2), (rows, 1), 0, top)
    return jnp.take_along_axis(listing, (jnp.arange(top)[None, :] + offset_by) % top, axis=1)


def portions_of(number_of, total, reach, lean, full):
    weights = [(1 << 20) // math.isqrt(rank ** lean) + 1 for rank in range(1, number_of + 1)]
    largest = reach if full else min(reach, max(-(-total // number_of), total * weights[0] // sum(weights)))
    least = 1 if total - largest >= number_of - 1 else 0
    counts, surplus = [largest] + [least] * (number_of - 1), total - largest - least * (number_of - 1)
    while surplus > 0:
        movable = [i for i in range(1, number_of) if counts[i] < largest] or [i for i in range(1, number_of) if counts[i] < reach]
        mass, left = sum([weights[i] for i in movable]), surplus
        for i in movable:
            addition = min(reach - counts[i], max(1, left * weights[i] // mass), surplus)
            counts[i] = counts[i] + addition
            surplus = surplus - addition
    return np.array(counts)


def centred(rng, dims, scale, limit, cuts=(), kind=jnp.bfloat16):
    entries = scale * jax.random.normal(rng, dims, jnp.float32)
    if cuts:
        entries = entries * block_scale(rng, dims, cuts, -0.22, 0.18)
    return jnp.clip(entries, -limit, limit).astype(kind)


def bell_draw_with(key, dims, width, limit, cuts, heavy, kind=jnp.bfloat16):
    entries = width * jax.random.normal(key, dims, jnp.float32)
    if cuts:
        entries = entries * block_scale(key, dims, cuts, -0.22, 0.18)
    return jnp.clip(with_spikes(entries, jax.random.fold_in(key, 3), *heavy), -limit, limit).astype(kind)


def setup_inputs(seed: int = 0) -> dict:
    keys = jax.random.split(jax.random.key(seed), 13)
    hidden = centred(keys[0], (TOKENS, D), 1.0, 6.0, ((0, 8),))
    cotangent = bell_draw_with(keys[1], (TOKENS, D), 1.0, 6.0, ((0, 8),), (0, 1, 8, 2.0))
    retained = centred(keys[2], (TOKENS, VW), 1.0, 6.0, ((0, 8), (1, 4)))
    queries = centred(keys[3], (TOKENS, H * DK), 0.25, 1.5, ((0, 8), (1, 4)))
    key_rows = centred(keys[4], (TOKENS, H * DK), 0.25, 1.5, ((0, 8), (1, 4)))
    value_rows = centred(keys[5], (TOKENS, VW), DV ** -0.5, 0.25, ((0, 8), (1, 4)))
    routes_keys = jax.random.split(jax.random.fold_in(keys[6], 1), TOKENS // TOK_DEV)
    routes_turns = jax.random.permutation(jax.random.fold_in(keys[6], 3), TOKENS // TOK_DEV)
    routes = jax.vmap(lambda own, number: assign_block(jax.random.fold_in(keys[6], 2), own, number, TOK_DEV, EXPERTS, TOP, CAP, 2))(routes_keys, routes_turns).reshape((TOKENS, TOP))
    route_weight = jnp.clip(0.2 + 1.3 * jax.random.uniform(keys[7], (TOKENS, TOP), jnp.float32) ** block_scale(keys[7], (TOKENS, TOP), ((0, 8),), -0.2, 0.2), 0.2, 1.5)
    gate_weight = centred(keys[8], (EXPERTS, D, FF), D ** -0.5, 0.125, ((0, 8), (2, 4)))
    up_weight = centred(keys[9], (EXPERTS, D, FF), D ** -0.5, 0.125, ((0, 8), (2, 4)))
    down_weight = centred(keys[10], (EXPERTS, FF, D), FF ** -0.5, 0.1875, ((0, 8), (1, 4)))
    out_weight = centred(keys[11], (D, VW), VW ** -0.5, 0.125, ((1, 4),))
    return dict(hidden=hidden, cotangent=cotangent, retained=retained, queries=queries, key_rows=key_rows, value_rows=value_rows, routes=routes, route_weight=route_weight, gate_weight=gate_weight, up_weight=up_weight, down_weight=down_weight, out_weight=out_weight)


def expert_backward(inputs, upstream, gate_matrix, up_matrix, down_matrix):
    gate_pre = jnp.dot(inputs, gate_matrix, preferred_element_type=jnp.float32)
    up_pre = jnp.dot(inputs, up_matrix, preferred_element_type=jnp.float32)
    sigma = jax.nn.sigmoid(gate_pre)
    active = gate_pre * sigma
    product = (active * up_pre).astype(jnp.bfloat16)
    down_part = jnp.dot(product.T, upstream, preferred_element_type=jnp.float32)
    unit_grad = jnp.dot(upstream, down_matrix.T, preferred_element_type=jnp.float32)
    gate_term = (unit_grad * up_pre * sigma * (1.0 + gate_pre * (1.0 - sigma))).astype(jnp.bfloat16)
    up_term = (unit_grad * active).astype(jnp.bfloat16)
    gate_part = jnp.dot(inputs.T, gate_term, preferred_element_type=jnp.float32)
    up_part = jnp.dot(inputs.T, up_term, preferred_element_type=jnp.float32)
    rows = gate_term.shape[0]
    group = FF // N_TP
    gate_split = gate_term.astype(jnp.float32).reshape(rows, N_TP, group)
    up_split = up_term.astype(jnp.float32).reshape(rows, N_TP, group)
    gate_cols = gate_matrix.astype(jnp.float32).reshape(D, N_TP, group)
    up_cols = up_matrix.astype(jnp.float32).reshape(D, N_TP, group)
    row_part = jnp.einsum('rnf,dnf->nrd', gate_split, gate_cols) + jnp.einsum('rnf,dnf->nrd', up_split, up_cols)
    return (gate_part, up_part, down_part, row_part.astype(jnp.bfloat16))

def slot_targets(routes):
    flat = routes.reshape(N_SP, TOK_DEV * TOP)
    onehot = (flat[:, :, None] == jnp.arange(EXPERTS, dtype=jnp.int32)[None, None, :]).astype(jnp.int32)
    rank = lax.optimization_barrier(jnp.sum(jnp.cumsum(onehot, axis=1) * onehot, axis=2)) - 1
    block = jnp.arange(N_SP, dtype=jnp.int32)[:, None]
    return (flat * (N_SP * CAP) + block * CAP + rank).reshape(-1).astype(jnp.int32)

def head_rates(head_ids, total_tokens):
    ids = head_ids.astype(jnp.float32)
    exponent = jnp.where(2 * head_ids < H, -5.0 - ids, -math.log2(total_tokens) - (ids - H // 2))
    log_gamma = jnp.log1p(-jnp.exp2(exponent))
    scale = jnp.sqrt(-jnp.expm1(2.0 * log_gamma))
    return (log_gamma, scale)

def span_states(query_three, key_three, value_three, output_grad_three, log_gamma):
    count = query_three.shape[0]
    place = jnp.arange(count, dtype=jnp.float32)[:, None]
    suffix_decay = jnp.exp(log_gamma[None, :] * (count - place))
    prefix_decay = jnp.exp(log_gamma[None, :] * (place + 1.0))
    head_position = lax.Precision.HIGHEST
    forward_sweep = jnp.einsum('ibz,ibm->bzm', key_three.astype(jnp.float32) * suffix_decay[:, :, None], value_three.astype(jnp.float32), precision=head_position)
    backward_sweep = jnp.einsum('stz,stb->tzb', query_three.astype(jnp.float32) * prefix_decay[:, :, None], output_grad_three.astype(jnp.float32), precision=head_position)
    return (forward_sweep, backward_sweep)

def span_grads(query_three, key_three, value_three, output_grad_three, prior_positions, later_positions, log_gamma, scale):
    count = query_three.shape[0]
    head_position = lax.Precision.HIGHEST
    query_flat, key_flat, value_flat, output_grad_flat = (query_three.astype(jnp.float32), key_three.astype(jnp.float32), value_three.astype(jnp.float32), output_grad_three.astype(jnp.float32))
    place = jnp.arange(count, dtype=jnp.float32)
    gap = place[:, None] - place[None, :]
    weight = jnp.where(gap[None] >= 0, scale[:, None, None] * jnp.exp(log_gamma[:, None, None] * jnp.maximum(gap, 0.0)[None]), 0.0)
    local_value_grad = (jnp.einsum('ihv,jhv->hij', output_grad_flat, value_flat) * weight).astype(jnp.bfloat16).astype(jnp.float32)
    local_query_key = (jnp.einsum('ihd,jhd->hij', query_flat, key_flat) * weight).astype(jnp.bfloat16).astype(jnp.float32)
    leading_span = (scale[None, :] * jnp.exp(log_gamma[None, :] * place[:, None]))[:, :, None]
    trailing_span = (scale[None, :] * jnp.exp(log_gamma[None, :] * (count - 1.0 - place[:, None])))[:, :, None]
    query_piece = jnp.einsum('zby,yze->bze', local_value_grad, key_flat) + leading_span * jnp.einsum('eal,gel->gea', prior_positions, output_grad_flat, precision=head_position)
    key_piece = jnp.einsum('lcx,clo->xlo', local_value_grad, query_flat) + trailing_span * jnp.einsum('gta,wga->wgt', later_positions, value_flat, precision=head_position)
    value_piece = jnp.einsum('upb,puk->buk', local_query_key, output_grad_flat) + trailing_span * jnp.einsum('tdx,btd->btx', later_positions, key_flat, precision=head_position)
    return (query_piece, key_piece, value_piece)

def reference(hidden, cotangent, retained, queries, key_rows, value_rows, routes, route_weight, gate_weight, up_weight, down_weight, out_weight):
    target = slot_targets(routes)
    slots = EXPERTS * N_SP * CAP
    upstream = (route_weight[:, :, None] * cotangent[:, None, :].astype(jnp.float32)).astype(jnp.bfloat16).reshape(-1, D)
    inputs = jnp.repeat(hidden, TOP, axis=0)
    up_buffer = jnp.zeros((slots, D), jnp.bfloat16).at[target].set(upstream).reshape(EXPERTS, N_SP * CAP, D)
    in_buffer = jnp.zeros((slots, D), jnp.bfloat16).at[target].set(inputs).reshape(EXPERTS, N_SP * CAP, D)
    gate_grad, up_grad, down_grad, row_grad = lax.map(lambda item: expert_backward(*item), (in_buffer, up_buffer, gate_weight, up_weight, down_weight))
    row_sum = lax.optimization_barrier(jnp.sum(row_grad.astype(jnp.float32), axis=1))
    routed = row_sum.reshape(slots, D)[target].reshape(TOKENS, TOP, D).sum(axis=1)
    layer_grad = (cotangent.astype(jnp.float32) + routed).astype(jnp.bfloat16)
    proj_grad = jnp.dot(layer_grad.T, retained, preferred_element_type=jnp.float32)
    mixed_grad = jnp.dot(layer_grad, out_weight, preferred_element_type=jnp.float32).astype(jnp.bfloat16)
    log_gamma, scale = head_rates(jnp.arange(H, dtype=jnp.int32), TOKENS)
    q5 = queries.reshape(N_SP, TOK_DEV, H, DK)
    k5 = key_rows.reshape(N_SP, TOK_DEV, H, DK)
    v5 = value_rows.reshape(N_SP, TOK_DEV, H, DV)
    do5 = mixed_grad.reshape(N_SP, TOK_DEV, H, DV)
    forward_shard_local, backward_local = lax.map(lambda item: span_states(*item, log_gamma), (q5, k5, v5, do5))
    decay_span = jnp.exp(log_gamma * TOK_DEV)[:, None, None]

    def carry_step(carry, local):
        return (carry * decay_span + local, carry)
    empty = jnp.zeros((H, DK, DV), jnp.float32)
    _, before_all = lax.scan(carry_step, empty, forward_shard_local)
    _, after_all = lax.scan(carry_step, empty, backward_local, reverse=True)
    query_gradient, key_gradient, value_gradient = lax.map(lambda item: span_grads(*item, log_gamma, scale), (q5, k5, v5, do5, before_all, after_all))
    return (gate_grad, up_grad, down_grad, proj_grad, query_gradient.reshape(TOKENS, H * DK), key_gradient.reshape(TOKENS, H * DK), value_gradient.reshape(TOKENS, H * DV))
```

```python
import functools
import math

import jax
import jax.numpy as jnp
from jax import lax
from jax.experimental import pallas as pl
from jax.experimental.pallas import tpu as pltpu
from jax.sharding import PartitionSpec as P

H = 4
DK = 256
DV = 512
GROUPS = 4
MESH = pl.DeviceIdType.MESH
ROWS = (((0,), (0,)), ((), ()))
COLS = (((1,), (1,)), ((), ()))


def dot(a, b, dims=(((1,), (0,)), ((), ()))):
    return lax.dot_general(a, b, dims, preferred_element_type=jnp.float32)


def carried(part, log_span, axis, reverse):
    count = lax.axis_size(axis)
    held = part
    ahead = jnp.zeros_like(part)
    step = 1
    while step < count:
        pairs = [(i + step, i) if reverse else (i, i + step) for i in range(count - step)]
        got = lax.ppermute(held.astype(jnp.bfloat16), axis, pairs).astype(jnp.float32)
        ahead = ahead + jnp.exp(log_span * (step - 1.0))[:, None, None] * got
        held = held + jnp.exp(log_span * float(step))[:, None, None] * got
        step *= 2
    return ahead


def moe_kernel(
    count,
    place_ref,
    rw_ref,
    hid_ref,
    cot_ref,
    wg_hbm,
    wu_hbm,
    wd_hbm,
    layer_out,
    gg_ref,
    ug_ref,
    dg_ref,
    wg,
    wu,
    wd,
    packed,
    packed2,
    got,
    terms,
    part,
    half,
    kept,
    moving,
    other,
    ret,
    total,
    layer,
    wsem,
    d_s,
    d_r,
    a_s,
    a_r,
    b_s,
    b_r,
    c_s,
    c_r,
    h_s,
    h_r,
    x_s,
    x_r,
    r_s,
    r_r,
    la_s,
    la_r,
    lb_s,
    lb_r,
    lc_s,
    lc_r,
):
    sp = lax.axis_index("sp")
    tp = lax.axis_index("tp")
    cap = place_ref.shape[1]
    wide = hid_ref.shape[1] // 4
    per = count // GROUPS
    offs = [pl.multiple_of(jnp.bitwise_xor(tp, r) * wide, wide) for r in range(4)]
    cols = [pl.ds(o, wide) for o in offs]

    loads = [
        pltpu.make_async_copy(src, dst, wsem.at[i])
        for i, (src, dst) in enumerate(((wg_hbm, wg), (wu_hbm, wu), (wd_hbm, wd)))
    ]
    for load in loads:
        load.start()

    def along_sp(m, src, dst, s, r):
        peer = (jnp.bitwise_xor(sp, m), tp)
        return pltpu.make_async_remote_copy(src, dst, s, r, device_id=peer, device_id_type=MESH)

    def along_tp(m, src, dst, s, r):
        peer = (sp, jnp.bitwise_xor(tp, m))
        return pltpu.make_async_remote_copy(src, dst, s, r, device_id=peer, device_id_type=MESH)

    barrier = pltpu.get_barrier_semaphore()
    for m in range(1, count):
        pl.semaphore_signal(
            barrier, inc=1, device_id=(jnp.bitwise_xor(sp, m), tp), device_id_type=MESH
        )
    for m in (1, 2):
        pl.semaphore_signal(
            barrier, inc=1, device_id=(sp, jnp.bitwise_xor(tp, m)), device_id_type=MESH
        )

    def pack(m, r):
        one = place_ref[jnp.bitwise_xor(sp, m)]
        rows = dot(one, hid_ref[:, cols[r]]).astype(jnp.bfloat16)
        ups = rw_ref[jnp.bitwise_xor(sp, m)] * dot(one, cot_ref[:, cols[r]])
        return rows, ups.astype(jnp.bfloat16)

    def stored(ref, pair):
        ref[0], ref[1] = pair

    sends = []

    def begin(copy):
        copy.start()
        sends.append(copy)
        return copy

    stored(packed.at[1], pack(1, 0))
    stored(packed2, pack(1, 2))
    pl.semaphore_wait(barrier, count + 1)
    arrive = {}
    arrive2 = begin(along_sp(1, packed2, got.at[2, :, 1], d_s.at[0], d_r.at[0]))
    for m in range(1, count):
        if m > 1:
            stored(packed.at[m], pack(m, 0))
        arrive[m] = begin(along_sp(m, packed.at[m], got.at[0, :, m], d_s.at[m], d_r.at[m]))
    for r in range(4):
        rows, ups = pack(0, r)
        got[r, 0, 0] = rows
        got[r, 1, 0] = ups

    from_pair, from_x, from_diag = {}, {}, {}

    def relay_first(m):
        arrive[m].wait_recv()
        from_pair[m] = begin(along_tp(1, got.at[0, :, m], got.at[1, :, m], a_s.at[m], a_r.at[m]))
        if m > 1:
            from_x[m] = begin(along_tp(2, got.at[0, :, m], got.at[2, :, m], b_s.at[m], b_r.at[m]))

    def relay_second(m):
        if m > 1:
            from_x[m].wait_recv()
        else:
            arrive2.wait_recv()
        from_diag[m] = begin(along_tp(1, got.at[2, :, m], got.at[3, :, m], c_s.at[m], c_r.at[m]))

    def rows_of(a, r, g):
        return got[r, a, g * per : (g + 1) * per].reshape(per * cap, wide)

    halves, across = {}, {}
    n = per * cap

    def expert(g):
        for m in range(max(1, g * per), (g + 1) * per):
            from_pair[m].wait_recv()
            from_diag[m].wait_recv()
        gate_pre = sum(dot(rows_of(0, r, g), wg[cols[r], :]) for r in range(4))
        up_pre = sum(dot(rows_of(0, r, g), wu[cols[r], :]) for r in range(4))
        unit = sum(dot(rows_of(1, r, g), wd[:, cols[r]], COLS) for r in range(4))
        sigma = jax.nn.sigmoid(gate_pre)
        active = gate_pre * sigma
        span = pl.ds(g * n, n)
        terms[0, span] = (active * up_pre).astype(jnp.bfloat16)
        gate_term = (unit * up_pre * sigma * (1.0 + gate_pre * (1.0 - sigma))).astype(jnp.bfloat16)
        up_term = (unit * active).astype(jnp.bfloat16)
        terms[1, span] = gate_term
        terms[2, span] = up_term
        for at, r in ((2, 1), (3, 3), (0, 0), (1, 2)):
            piece = dot(gate_term, wg[cols[r], :], COLS) + dot(up_term, wu[cols[r], :], COLS)
            part[at, span] = piece.astype(jnp.bfloat16)
            if at == 3:
                halves[g] = begin(
                    along_tp(1, part.at[2:4, span], half.at[:, span], h_s.at[g], h_r.at[g])
                )

    def cross(g):
        span = pl.ds(g * n, n)
        halves[g].wait_recv()
        mine = part[1, span].astype(jnp.float32) + half[1, span].astype(jnp.float32)
        moving[span] = mine.astype(jnp.bfloat16)
        across[g] = begin(along_tp(2, moving.at[span], other.at[span], x_s.at[g], x_r.at[g]))
        mine = part[0, span].astype(jnp.float32) + half[0, span].astype(jnp.float32)
        kept[span] = mine.astype(jnp.bfloat16)

    back = {}

    def give_back(g):
        across[g].wait_recv()
        for m in range(g * per, (g + 1) * per):
            span = pl.ds(m * cap, cap)
            done = kept[span].astype(jnp.float32) + other[span].astype(jnp.float32)
            if m == 0:
                ret[0] = done.astype(jnp.bfloat16)
            else:
                kept[span] = done.astype(jnp.bfloat16)
                back[m] = begin(along_sp(m, kept.at[span], ret.at[m], r_s.at[m], r_r.at[m]))

    for m in range(1, per):
        relay_first(m)
        relay_second(m)
    for load in loads:
        load.wait()
    for g in range(1, GROUPS):
        for m in range(g * per, (g + 1) * per):
            relay_first(m)
            if m > g * per:
                relay_second(m - 1)
        expert(g - 1)
        relay_second((g + 1) * per - 1)
        cross(g - 1)
        if g > 1:
            give_back(g - 2)
    expert(GROUPS - 1)
    give_back(GROUPS - 2)
    cross(GROUPS - 1)

    def whole(a, r):
        return got[r, a].reshape(count * cap, wide)

    for r in range(4):
        dg_ref[:, cols[r]] = dot(terms[0], whole(1, r), ROWS)
    give_back(GROUPS - 1)
    for r in range(4):
        gg_ref[cols[r], :] = dot(whole(0, r), terms[1], ROWS)
        ug_ref[cols[r], :] = dot(whole(0, r), terms[2], ROWS)
    total[...] = cot_ref[:, cols[0]].astype(jnp.float32)
    for m in range(count):
        if m:
            back[m].wait_recv()
        total[...] += dot(place_ref[jnp.bitwise_xor(sp, m)], ret[m], ROWS)
    layer[0] = total[...].astype(jnp.bfloat16)
    one = begin(along_tp(2, layer.at[0], layer.at[2], lb_s, lb_r))
    two = begin(along_tp(1, layer.at[0], layer.at[1], la_s, la_r))
    one.wait_recv()
    three = begin(along_tp(1, layer.at[2], layer.at[3], lc_s, lc_r))
    two.wait_recv()
    three.wait_recv()
    for r in range(4):
        layer_out[:, cols[r]] = layer[r]
    for copy in sends:
        copy.wait_send()


def moe(place, row_weight, hidden, cotangent, gate_w, up_w, down_w):
    count = lax.axis_size("sp")
    assert lax.axis_size("tp") == 4 and count % GROUPS == 0
    experts, cap, tokens = place.shape
    width = hidden.shape[1]
    units = gate_w.shape[1]
    wide = width // 4
    rows = count * cap
    bf, f32 = jnp.bfloat16, jnp.float32
    dma = pltpu.SemaphoreType.DMA
    vmem = pl.BlockSpec(memory_space=pltpu.VMEM)
    hbm = pl.BlockSpec(memory_space=pl.ANY)
    return pl.pallas_call(
        functools.partial(moe_kernel, count),
        out_shape=(
            jax.ShapeDtypeStruct((tokens, width), bf),
            jax.ShapeDtypeStruct((width, units), f32),
            jax.ShapeDtypeStruct((width, units), f32),
            jax.ShapeDtypeStruct((units, width), f32),
        ),
        in_specs=[vmem] * 4 + [hbm] * 3,
        out_specs=(vmem,) * 4,
        scratch_shapes=[
            pltpu.VMEM((width, units), bf),
            pltpu.VMEM((width, units), bf),
            pltpu.VMEM((units, width), bf),
            pltpu.VMEM((count, 2, cap, wide), bf),
            pltpu.VMEM((2, cap, wide), bf),
            pltpu.VMEM((4, 2, count, cap, wide), bf),
            pltpu.VMEM((3, rows, units), bf),
            pltpu.VMEM((4, rows, wide), bf),
            pltpu.VMEM((2, rows, wide), bf),
            pltpu.VMEM((rows, wide), bf),
            pltpu.VMEM((rows, wide), bf),
            pltpu.VMEM((rows, wide), bf),
            pltpu.VMEM((count, cap, wide), bf),
            pltpu.VMEM((tokens, wide), f32),
            pltpu.VMEM((4, tokens, wide), bf),
            dma((3,)),
        ]
        + [dma((count,))] * 8
        + [dma((GROUPS,))] * 4
        + [dma((count,))] * 2
        + [dma] * 6,
        compiler_params=pltpu.CompilerParams(
            collective_id=0, has_side_effects=True, vmem_limit_bytes=60 * 2**20
        ),
        name="moe",
    )(place, row_weight, hidden, cotangent, gate_w, up_w, down_w)


def head_rates(head_ids, total_tokens):
    ids = head_ids.astype(jnp.float32)
    exponent = jnp.where(2 * head_ids < H, -5.0 - ids, -math.log2(total_tokens) - (ids - H // 2))
    log_gamma = jnp.log1p(-jnp.exp2(exponent))
    scale = jnp.sqrt(-jnp.expm1(2.0 * log_gamma))
    return (log_gamma, scale)


def routing(routes, route_weight, experts_all, tok_local):
    top_count = routes.shape[1]
    capacity = 3 * tok_local * top_count // (2 * experts_all)
    capacity = -(-capacity // 16) * 16
    ids = jnp.arange(experts_all, dtype=jnp.int32)[:, None]
    named = [routes[:, r][None, :] == ids for r in range(top_count)]
    member = sum(m.astype(jnp.float32) for m in named)
    slot_weight = sum(jnp.where(m, route_weight[:, r][None, :], 0.0) for r, m in enumerate(named))
    order = jnp.arange(tok_local, dtype=jnp.int32)
    earlier = (order[:, None] < order[None, :]).astype(jnp.bfloat16)
    rank = jnp.dot(member.astype(jnp.bfloat16), earlier, preferred_element_type=jnp.float32)
    rank = jnp.where(member > 0.0, rank, -1.0).astype(jnp.int32)
    hit = rank[:, None, :] == jnp.arange(capacity, dtype=jnp.int32)[None, :, None]
    row_weight = jnp.sum(jnp.where(hit, slot_weight[:, None, :], 0.0), axis=2, keepdims=True)
    return hit.astype(jnp.bfloat16), row_weight


def local(
    hidden,
    cotangent,
    retained,
    queries,
    key_rows,
    value_rows,
    routes,
    route_weight,
    gate_weight,
    up_weight,
    down_weight,
    out_weight,
):
    sp_count = lax.axis_size("sp")
    tp_count = lax.axis_size("tp")
    tok_local = hidden.shape[0]
    experts_all = gate_weight.shape[0] * sp_count
    assert gate_weight.shape[0] == 1
    place_rows, row_weight = routing(routes, route_weight, experts_all, tok_local)
    heads_local = queries.shape[1] // DK
    head_ids = lax.axis_index("tp") * heads_local + jnp.arange(heads_local, dtype=jnp.int32)
    log_gamma, scale = head_rates(head_ids, tok_local * sp_count)
    query_three = queries.reshape(tok_local, heads_local, DK)
    key_three = key_rows.reshape(tok_local, heads_local, DK)
    value_three = value_rows.reshape(tok_local, heads_local, DV)
    place = jnp.arange(tok_local, dtype=jnp.float32)
    suffix_decay = jnp.exp(log_gamma[None, :] * (tok_local - place[:, None]))
    prefix_decay = jnp.exp(log_gamma[None, :] * (place[:, None] + 1.0))
    forward_shard_local = jnp.einsum(
        "ibz,ibm->bzm",
        (key_three * suffix_decay[:, :, None]).astype(jnp.bfloat16),
        value_three,
        preferred_element_type=jnp.float32,
    )
    log_span = log_gamma * tok_local
    retained_all = lax.all_gather(retained, "sp", axis=0, tiled=True)
    layer_grad, gate_grad, up_grad, down_grad = moe(
        place_rows,
        row_weight,
        hidden,
        cotangent,
        gate_weight[0],
        up_weight[0],
        down_weight[0],
    )
    prior_positions = carried(forward_shard_local, log_span, "sp", False).astype(jnp.bfloat16)
    mixed_grad = jnp.dot(layer_grad, out_weight, preferred_element_type=jnp.float32).astype(
        jnp.bfloat16
    )
    share = tok_local // tp_count
    share_rows = lax.dynamic_slice_in_dim(layer_grad, lax.axis_index("tp") * share, share, 0)
    share_rows = share_rows.reshape(share, sp_count, -1).swapaxes(0, 1)
    block_rows = lax.all_to_all(share_rows, "sp", split_axis=0, concat_axis=0, tiled=True)
    block_all = lax.all_gather(block_rows, "tp", axis=1, tiled=True)
    proj_grad = lax.dot_general(
        block_all.reshape(sp_count * tok_local, -1),
        retained_all,
        (((0,), (0,)), ((), ())),
        preferred_element_type=jnp.float32,
    )
    output_grad_three = mixed_grad.reshape(tok_local, heads_local, DV)
    backward_local = jnp.einsum(
        "stz,stb->tzb",
        (query_three * prefix_decay[:, :, None]).astype(jnp.bfloat16),
        output_grad_three,
        preferred_element_type=jnp.float32,
    )
    later_positions = carried(backward_local, log_span, "sp", True).astype(jnp.bfloat16)
    gap = place[:, None] - place[None, :]
    weight = jnp.where(
        gap[None] >= 0,
        scale[:, None, None] * jnp.exp(log_gamma[:, None, None] * jnp.maximum(gap, 0.0)[None]),
        0.0,
    )
    local_value_grad = (
        jnp.einsum(
            "ihv,jhv->hij", output_grad_three, value_three, preferred_element_type=jnp.float32
        )
        * weight
    ).astype(jnp.bfloat16)
    local_query_key = (
        jnp.einsum("ihd,jhd->hij", query_three, key_three, preferred_element_type=jnp.float32)
        * weight
    ).astype(jnp.bfloat16)
    leading_span = (scale[None, :] * jnp.exp(log_gamma[None, :] * place[:, None]))[:, :, None]
    trailing_span = (
        scale[None, :] * jnp.exp(log_gamma[None, :] * (tok_local - 1.0 - place[:, None]))
    )[:, :, None]
    query_gradient = jnp.einsum(
        "zby,yze->bze", local_value_grad, key_three, preferred_element_type=jnp.float32
    )
    query_gradient = query_gradient + leading_span * jnp.einsum(
        "eal,gel->gea", prior_positions, output_grad_three, preferred_element_type=jnp.float32
    )
    key_gradient = jnp.einsum(
        "lcx,clo->xlo", local_value_grad, query_three, preferred_element_type=jnp.float32
    )
    key_gradient = key_gradient + trailing_span * jnp.einsum(
        "gta,wga->wgt", later_positions, value_three, preferred_element_type=jnp.float32
    )
    value_gradient = jnp.einsum(
        "upb,puk->buk", local_query_key, output_grad_three, preferred_element_type=jnp.float32
    )
    value_gradient = value_gradient + trailing_span * jnp.einsum(
        "tdx,btd->btx", later_positions, key_three, preferred_element_type=jnp.float32
    )
    return (
        gate_grad[None],
        up_grad[None],
        down_grad[None],
        proj_grad,
        query_gradient.reshape(tok_local, heads_local * DK),
        key_gradient.reshape(tok_local, heads_local * DK),
        value_gradient.reshape(tok_local, heads_local * DV),
    )


def solution(mesh):
    return jax.shard_map(
        local,
        mesh=mesh,
        in_specs=(
            P("sp", None),
            P("sp", None),
            P("sp", "tp"),
            P("sp", "tp"),
            P("sp", "tp"),
            P("sp", "tp"),
            P("sp", None),
            P("sp", None),
            P("sp", None, "tp"),
            P("sp", None, "tp"),
            P("sp", "tp", None),
            P(None, "tp"),
        ),
        out_specs=(
            P("sp", None, "tp"),
            P("sp", None, "tp"),
            P("sp", "tp", None),
            P("sp", "tp"),
            P("sp", "tp"),
            P("sp", "tp"),
            P("sp", "tp"),
        ),
        check_vma=False,
    )
```

```python
import functools
import math

import jax
import jax.numpy as jnp
from jax import lax
from jax.experimental import pallas as pl
from jax.experimental.pallas import tpu as pltpu
from jax.sharding import PartitionSpec as P

H = 4
DK = 256
DV = 512
GROUPS = 8
LINKS = 4
MESH = pl.DeviceIdType.MESH
ROWS = (((0,), (0,)), ((), ()))
COLS = (((1,), (1,)), ((), ()))


def dot(a, b, dims=(((1,), (0,)), ((), ()))):
    return lax.dot_general(a, b, dims, preferred_element_type=jnp.float32)


class Chain:
    def __init__(self, count, reverse, log_span, own, pair_in, summed, link_in, link_out, out_half,
                 state, sems):
        self.sp, self.tp = lax.axis_index("sp"), lax.axis_index("tp")
        self.y = self.sp % 2
        self.yy = self.y if reverse else 1 - self.y
        self.pairs = count // 2
        z = self.sp // 2
        self.t = self.pairs - 1 - z if reverse else z
        self.next = jnp.where(self.t < self.pairs - 1, self.sp - 2 if reverse else self.sp + 2, self.sp)
        self.decay = jnp.exp(jnp.full((8, 128), log_span, jnp.float32))[0:1, 0:1]
        self.own, self.pair_in, self.summed = own, pair_in, summed
        self.link_in, self.link_out, self.out_half, self.state = link_in, link_out, out_half, state
        self.ps, self.pr, self.ls, self.lr, self.bs, self.br = sems
        self.chunks = link_in.shape[0]
        self.wide = link_in.shape[2]

    def pair(self, src, dst, s, r):
        peer = (jnp.bitwise_xor(self.sp, 1), self.tp)
        return pltpu.make_async_remote_copy(src, dst, s, r, device_id=peer, device_id_type=MESH)

    def link(self, c):
        return pltpu.make_async_remote_copy(
            self.link_out.at[c],
            self.link_in.at[c],
            self.ls.at[c],
            self.lr.at[c],
            device_id=(self.next, self.tp),
            device_id_type=MESH,
        )

    def start(self):
        @pl.when(self.t == 0)
        def _():
            self.link_in[...] = jnp.zeros_like(self.link_in)

        self.one = self.pair(self.own.at[1 - self.y], self.pair_in, self.ps, self.pr)
        self.one.start()

    def fold(self):
        self.one.wait_recv()
        g = self.decay
        mine = jnp.where(self.yy == 0, 1.0, g) * self.own[self.y].astype(jnp.float32)
        theirs = jnp.where(self.yy == 0, g, 1.0) * self.pair_in[...].astype(jnp.float32)
        self.summed[...] = mine + theirs

    def step(self, i):
        if i >= self.pairs:
            return

        @pl.when(self.t == i)
        def _():
            for c in range(self.chunks):
                if i > 0:
                    self.link(c).wait_recv()
                if i < self.pairs - 1:
                    value = self.summed[:, c * self.wide : (c + 1) * self.wide]
                    if i > 0:
                        value = value + self.decay * self.decay * self.link_in[c].astype(jnp.float32)
                    self.link_out[c] = value.astype(jnp.bfloat16)
                    self.link(c).start()

    def finish(self):
        g = self.decay
        for c in range(self.chunks):
            cols = slice(c * self.wide, (c + 1) * self.wide)
            ahead = self.link_in[c].astype(jnp.float32)
            own = self.own[self.y, :, cols].astype(jnp.float32)
            near = self.pair_in[:, cols].astype(jnp.float32)
            mine = jnp.where(self.yy == 0, near + g * ahead, ahead)
            theirs = jnp.where(self.yy == 0, ahead, own + g * ahead)
            self.state[self.y, :, cols] = mine.astype(jnp.bfloat16)
            self.out_half[:, cols] = theirs.astype(jnp.bfloat16)
        self.two = self.pair(self.out_half, self.state.at[self.y], self.bs, self.br)
        self.two.start()

    def wait(self):
        self.pair(self.out_half, self.state.at[1 - self.y], self.bs, self.br).wait_recv()

    def drain(self):
        self.one.wait_send()
        self.two.wait_send()

        @pl.when(self.t < self.pairs - 1)
        def _():
            for c in range(self.chunks):
                self.link(c).wait_send()


def chain_scratch():
    half = DK // 2
    return [
        pltpu.VMEM((2, half, DV), jnp.bfloat16),
        pltpu.VMEM((half, DV), jnp.bfloat16),
        pltpu.VMEM((half, DV), jnp.float32),
        pltpu.VMEM((LINKS, half, DV // LINKS), jnp.bfloat16),
        pltpu.VMEM((LINKS, half, DV // LINKS), jnp.bfloat16),
        pltpu.VMEM((half, DV), jnp.bfloat16),
        pltpu.VMEM((2, half, DV), jnp.bfloat16),
        pltpu.SemaphoreType.DMA,
        pltpu.SemaphoreType.DMA,
        pltpu.SemaphoreType.DMA((LINKS,)),
        pltpu.SemaphoreType.DMA((LINKS,)),
        pltpu.SemaphoreType.DMA,
        pltpu.SemaphoreType.DMA,
    ]


def rates(tokens):
    tp = lax.axis_index("tp")
    logs, scales = [], []
    for h in range(H):
        exponent = -5.0 - h if 2 * h < H else -math.log2(tokens) - (h - H // 2)
        logs.append(math.log1p(-(2.0**exponent)))
        scales.append(math.sqrt(-math.expm1(2.0 * logs[-1])))
    log_gamma, scale = jnp.float32(logs[0]), jnp.float32(scales[0])
    for h in range(1, H):
        log_gamma = jnp.where(tp == h, jnp.float32(logs[h]), log_gamma)
        scale = jnp.where(tp == h, jnp.float32(scales[h]), scale)
    return log_gamma, scale


def positions(shape, axis):
    return lax.broadcasted_iota(jnp.int32, shape, axis).astype(jnp.float32)


def layer_kernel(
    count,
    place_ref,
    rw_ref,
    hid_ref,
    cot_ref,
    q_ref,
    k_ref,
    v_ref,
    wg_hbm,
    wu_hbm,
    wd_hbm,
    wo_hbm,
    kept_hbm,
    gg_ref,
    ug_ref,
    dg_ref,
    pg_ref,
    qg_ref,
    kg_ref,
    vg_ref,
    gg,
    ug,
    dg,
    pg,
    qg,
    kg,
    vg,
    wg,
    wu,
    wd,
    wo,
    packed,
    packed2,
    got,
    terms,
    part,
    half,
    kept,
    moving,
    other,
    ret,
    total,
    layer,
    spread,
    mixed_ref,
    flipped,
    blocks,
    near_v,
    near_k,
    load_sem,
    store_sem,
    d_s,
    d_r,
    a_s,
    a_r,
    b_s,
    b_r,
    c_s,
    c_r,
    r_s,
    r_r,
    k_s,
    k_r,
    p_s,
    p_r,
    h_s,
    h_r,
    x_s,
    x_r,
    l_s,
    l_r,
    *chain_refs,
):
    sp = lax.axis_index("sp")
    tp = lax.axis_index("tp")
    bf = jnp.bfloat16
    cap = place_ref.shape[1]
    tokens, width = hid_ref.shape
    wide = width // 4
    per = count // GROUPS
    n = per * cap
    offs = [pl.multiple_of(jnp.bitwise_xor(tp, r) * wide, wide) for r in range(4)]
    cols = [pl.ds(o, wide) for o in offs]

    places = ((wg_hbm, wg), (wu_hbm, wu), (wd_hbm, wd), (wo_hbm, wo), (kept_hbm, spread.at[0]))
    loads = [pltpu.make_async_copy(src, dst, load_sem.at[i]) for i, (src, dst) in enumerate(places)]
    for load in loads:
        load.start()

    def along_sp(m, src, dst, s, r):
        peer = (jnp.bitwise_xor(sp, m), tp)
        return pltpu.make_async_remote_copy(src, dst, s, r, device_id=peer, device_id_type=MESH)

    def along_tp(m, src, dst, s, r):
        peer = (sp, jnp.bitwise_xor(tp, m))
        return pltpu.make_async_remote_copy(src, dst, s, r, device_id=peer, device_id_type=MESH)

    barrier = pltpu.get_barrier_semaphore()
    for m in range(1, count):
        pl.semaphore_signal(
            barrier, inc=1, device_id=(jnp.bitwise_xor(sp, m), tp), device_id_type=MESH
        )
    for m in (1, 2):
        pl.semaphore_signal(
            barrier, inc=1, device_id=(sp, jnp.bitwise_xor(tp, m)), device_id_type=MESH
        )

    sends = []

    def begin(copy):
        copy.start()
        sends.append(copy)
        return copy

    def pack(m, r):
        one = place_ref[jnp.bitwise_xor(sp, m)]
        rows = dot(one, hid_ref[:, cols[r]]).astype(bf)
        ups = rw_ref[jnp.bitwise_xor(sp, m)] * dot(one, cot_ref[:, cols[r]])
        return rows, ups.astype(bf)

    packed2[0], packed2[1] = pack(1, 2)
    arrive = {}
    for m in range(1, count):
        packed[m, 0], packed[m, 1] = pack(m, 0)
        if m == 1:
            pl.semaphore_wait(barrier, count + 1)
        arrive[m] = begin(along_sp(m, packed.at[m], got.at[0, :, m], d_s.at[m], d_r.at[m]))
        if m == 1:
            arrive2 = begin(along_sp(1, packed2, got.at[2, :, 1], d_s.at[0], d_r.at[0]))
    for r in range(4):
        got[r, 0, 0], got[r, 1, 0] = pack(0, r)

    log_gamma, scale = rates(tokens * count)
    set_size = len(chain_refs) // 2
    refs = chain_refs[:set_size]
    chain = Chain(count, False, log_gamma * tokens, *refs[:7], refs[7:])
    prior_ref = refs[6]
    faded = k_ref[...] * jnp.exp(log_gamma * (tokens - positions((tokens, DK), 0)))
    refs[0][...] = dot(faded.astype(bf), v_ref[...], ROWS).astype(bf).reshape(refs[0].shape)
    chain.start()

    spreads, seen = {}, set()

    def landed(s):
        if s and s not in seen:
            seen.add(s)
            spreads[s].wait_recv()

    def pass_on(s, bits):
        landed(s)
        for bit in bits:
            to = s | bit
            spreads[to] = begin(along_sp(bit, spread.at[s], spread.at[to], k_s.at[to], k_r.at[to]))

    far = count // 2
    near_bits = [1 << i for i in range(far.bit_length() - 1)][::-1]
    loads[4].wait()
    pass_on(0, near_bits)

    from_pair, from_x, from_diag = {}, {}, {}

    def relay_first(m):
        arrive[m].wait_recv()
        if m > 1:
            from_x[m] = begin(along_tp(2, got.at[0, :, m], got.at[2, :, m], b_s.at[m], b_r.at[m]))
        from_pair[m] = begin(along_tp(1, got.at[0, :, m], got.at[1, :, m], a_s.at[m], a_r.at[m]))

    def relay_second(m):
        if m > 1:
            from_x[m].wait_recv()
        else:
            arrive2.wait_recv()
        from_diag[m] = begin(along_tp(1, got.at[2, :, m], got.at[3, :, m], c_s.at[m], c_r.at[m]))

    def slots(g):
        return range(max(1, g * per), (g + 1) * per)

    def rows_of(a, r, g):
        return got[r, a, g * per : (g + 1) * per].reshape(n, wide)

    halves, across, back = {}, {}, {}

    def expert(g):
        for m in slots(g):
            from_pair[m].wait_recv()
            from_diag[m].wait_recv()
        gate_pre = sum(dot(rows_of(0, r, g), wg[cols[r], :]) for r in range(4))
        up_pre = sum(dot(rows_of(0, r, g), wu[cols[r], :]) for r in range(4))
        unit = sum(dot(rows_of(1, r, g), wd[:, cols[r]], COLS) for r in range(4))
        sigma = jax.nn.sigmoid(gate_pre)
        active = gate_pre * sigma
        span = pl.ds(g * n, n)
        terms[0, span] = (active * up_pre).astype(bf)
        gate_term = (unit * up_pre * sigma * (1.0 + gate_pre * (1.0 - sigma))).astype(bf)
        up_term = (unit * active).astype(bf)
        terms[1, span] = gate_term
        terms[2, span] = up_term
        for at, r in ((2, 1), (3, 3), (0, 0), (1, 2)):
            piece = dot(gate_term, wg[cols[r], :], COLS) + dot(up_term, wu[cols[r], :], COLS)
            part[at, span] = piece.astype(bf)
            if at == 3:
                halves[g] = begin(
                    along_tp(1, part.at[2:4, span], half.at[:, span], h_s.at[g], h_r.at[g])
                )

    def cross(g):
        span = pl.ds(g * n, n)
        halves[g].wait_recv()
        mine = part[1, span].astype(jnp.float32) + half[1, span].astype(jnp.float32)
        moving[span] = mine.astype(bf)
        across[g] = begin(along_tp(2, moving.at[span], other.at[span], x_s.at[g], x_r.at[g]))
        mine = part[0, span].astype(jnp.float32) + half[0, span].astype(jnp.float32)
        kept[span] = mine.astype(bf)

    def give_back(g):
        across[g].wait_recv()
        for m in range(g * per, (g + 1) * per):
            span = pl.ds(m * cap, cap)
            done = (kept[span].astype(jnp.float32) + other[span].astype(jnp.float32)).astype(bf)
            if m == 0:
                ret[0] = done
            else:
                kept[span] = done
                back[m] = begin(along_sp(m, kept.at[span], ret.at[m], r_s.at[m], r_r.at[m]))

    for m in slots(0):
        relay_first(m)
        relay_second(m)
    for load in loads[:4]:
        load.wait()
    expert(0)
    middle = GROUPS // 2
    for i in range(1, GROUPS):
        for m in slots(i):
            relay_first(m)
        if i > 1:
            for m in slots(i - 1):
                relay_second(m)
        if i > 2:
            give_back(i - 3)
        if i > 1:
            cross(i - 2)
            expert(i - 1)
        if i == middle + 1:
            pass_on(0, [far])
        if i == 3:
            chain.fold()
        if 3 <= i:
            chain.step(i - 3)
    last = GROUPS - 1
    for j in range(last - 2, count // 2):
        chain.step(j)
    for s in sorted(range(2, far, 2), key=lambda s: bin(s).count("1")):
        low = s & -s
        pass_on(s, [b for b in near_bits if b < low])
    cross(last - 1)
    for m in slots(last):
        relay_second(m)
    give_back(last - 2)
    chain.finish()
    expert(last)
    give_back(last - 1)
    pass_on(far, near_bits)
    cross(last)

    def whole(a, r):
        return got[r, a].reshape(count * cap, wide)

    for r in range(4):
        dg[:, cols[r]] = dot(terms[0], whole(1, r), ROWS)
    give_back(last)
    stores = []

    def store(src, dst):
        stores.append(pltpu.make_async_copy(src, dst, store_sem.at[len(stores)]))
        stores[-1].start()

    store(dg, dg_ref)
    total[...] = cot_ref[:, cols[0]].astype(jnp.float32)
    for m in range(count):
        if m:
            back[m].wait_recv()
        total[...] += dot(place_ref[jnp.bitwise_xor(sp, m)], ret[m], ROWS)
    layer[0] = total[...].astype(bf)
    one = begin(along_tp(2, layer.at[0], layer.at[2], l_s.at[0], l_r.at[0]))
    two = begin(along_tp(1, layer.at[0], layer.at[1], l_s.at[1], l_r.at[1]))

    step = min(256, wide)
    eye = (positions((step, step), 0) == positions((step, step), 1)).astype(bf)

    def flip(r):
        for c in range(wide // step):
            at = pl.multiple_of(offs[r] + c * step, step)
            flipped[pl.ds(at, step), :] = dot(eye, layer[r, :, c * step : (c + 1) * step], COLS).astype(bf)

    total[...] = dot(layer[0], wo[cols[0], :])
    flip(0)
    two.wait_recv()
    total[...] += dot(layer[1], wo[cols[1], :])
    flip(1)
    faded = (q_ref[...] * jnp.exp(log_gamma * (positions((tokens, DK), 0) + 1.0))).astype(bf)
    for r in range(4):
        gg[cols[r], :] = dot(whole(0, r), terms[1], ROWS)
    store(gg, gg_ref)
    for s in sorted(range(far + 2, count, 2), key=lambda s: bin(s).count("1")):
        low = s & -s
        pass_on(s, [b for b in near_bits if b < low])
    one.wait_recv()
    three = begin(along_tp(1, layer.at[2], layer.at[3], l_s.at[2], l_r.at[2]))
    total[...] += dot(layer[2], wo[cols[2], :])
    flip(2)
    three.wait_recv()
    mixed_ref[...] = (total[...] + dot(layer[3], wo[cols[3], :])).astype(bf)
    refs = chain_refs[set_size:]
    ahead = Chain(count, True, log_gamma * tokens, *refs[:7], refs[7:])
    refs[0][...] = dot(faded, mixed_ref[...], ROWS).astype(bf).reshape(refs[0].shape)
    ahead.start()
    flip(3)
    rows = width // count
    share = rows // 4
    for m in range(count):
        at = pl.multiple_of(jnp.bitwise_xor(sp, m) * rows + tp * share, share)
        if m:
            arrive[m] = begin(
                along_sp(m, flipped.at[pl.ds(at, share)], blocks.at[m, 0], p_s.at[m], p_r.at[m])
            )
        else:
            blocks[0, 0] = flipped[pl.ds(at, share)]
    for r in range(4):
        ug[cols[r], :] = dot(whole(0, r), terms[2], ROWS)
    store(ug, ug_ref)
    ahead.fold()
    ahead.step(0)
    gap = positions((tokens, tokens), 0) - positions((tokens, tokens), 1)
    fade = jnp.where(gap >= 0, scale * jnp.exp(log_gamma * jnp.maximum(gap, 0.0)), 0.0)
    near_v[...] = (dot(mixed_ref[...], v_ref[...], COLS) * fade).astype(bf)
    near_k[...] = (dot(q_ref[...], k_ref[...], COLS) * fade).astype(bf)
    ahead.step(1)
    lead = scale * jnp.exp(log_gamma * positions((tokens, DK), 0))
    chain.wait()
    prior = prior_ref[...].reshape(DK, DV)
    qg[...] = dot(near_v[...], k_ref[...]) + lead * dot(mixed_ref[...], prior, COLS)
    store(qg, qg_ref)
    kg[...] = dot(near_v[...], q_ref[...], ROWS)
    vg[...] = dot(near_k[...], mixed_ref[...], ROWS)
    for m in range(1, count):
        arrive[m].wait_recv()
    over_x = begin(along_tp(2, blocks.at[:, 0], blocks.at[:, 2], l_s.at[3], l_r.at[3]))
    over_pair = begin(along_tp(1, blocks.at[:, 0], blocks.at[:, 1], l_s.at[4], l_r.at[4]))
    for i in range(2, count // 2 - 1):
        ahead.step(i)
    ahead.step(count // 2 - 1)
    ahead.finish()
    over_x.wait_recv()
    diag = begin(along_tp(1, blocks.at[:, 2], blocks.at[:, 3], l_s.at[5], l_r.at[5]))
    over_pair.wait_recv()
    diag.wait_recv()
    for s in spreads:
        landed(s)
    proj = jnp.zeros((rows, spread.shape[2]), jnp.float32)
    for m in range(count):
        proj = proj + dot(blocks[m].reshape(rows, tokens), spread[m])
    proj = proj.reshape(4, share, spread.shape[2])
    for r in range(4):
        at = pl.multiple_of(jnp.bitwise_xor(tp, r) * share, share)
        pg[pl.ds(at, share), :] = proj[r]
    store(pg, pg_ref)
    ahead.wait()
    later = refs[6][...].reshape(DK, DV)
    trail = scale * jnp.exp(log_gamma * (tokens - 1.0 - positions((tokens, DV), 0)))
    kg[...] += trail[:, :DK] * dot(v_ref[...], later, COLS)
    store(kg, kg_ref)
    vg[...] += trail * dot(k_ref[...], later)
    store(vg, vg_ref)
    for copy in sends:
        copy.wait_send()
    chain.drain()
    ahead.drain()
    for copy in stores:
        copy.wait()


def publish_kernel(count, *refs):
    srcs, dsts, tmps, sems = refs[:count], refs[count : 2 * count], refs[2 * count : -1], refs[-1]
    ins = [pltpu.make_async_copy(srcs[i], tmps[i], sems.at[0, i]) for i in range(count)]
    outs = [pltpu.make_async_copy(tmps[i], dsts[i], sems.at[1, i]) for i in range(count)]
    for copy in ins:
        copy.start()
    for i in range(count):
        ins[i].wait()
        outs[i].start()
    for copy in outs:
        copy.wait()


def publish(*arrays):
    hbm = pl.BlockSpec(memory_space=pl.ANY)
    count = len(arrays)
    return pl.pallas_call(
        functools.partial(publish_kernel, count),
        out_shape=tuple(jax.ShapeDtypeStruct(a.shape, a.dtype) for a in arrays),
        in_specs=[hbm] * count,
        out_specs=(hbm,) * count,
        scratch_shapes=[pltpu.VMEM(a.shape, a.dtype) for a in arrays]
        + [pltpu.SemaphoreType.DMA((2, count))],
        compiler_params=pltpu.CompilerParams(vmem_limit_bytes=62 * 2**20),
        name="publish",
    )(*arrays)


def whole_layer(
    place, row_weight, hidden, cotangent, queries, keys, values, gate_w, up_w, down_w, out_w, retained
):
    count = lax.axis_size("sp")
    assert lax.axis_size("tp") == 4 and count % GROUPS == 0
    cap = place.shape[1]
    tokens, width = hidden.shape
    units = gate_w.shape[1]
    wide = width // 4
    slots = count * cap
    rows, vals = width // count, retained.shape[1]
    bf, f32 = jnp.bfloat16, jnp.float32
    dma = pltpu.SemaphoreType.DMA
    vmem = pl.BlockSpec(memory_space=pltpu.VMEM)
    hbm = pl.BlockSpec(memory_space=pl.ANY)
    shape = jax.ShapeDtypeStruct
    return pl.pallas_call(
        functools.partial(layer_kernel, count),
        out_shape=(
            shape((width, units), f32),
            shape((width, units), f32),
            shape((units, width), f32),
            shape((rows, vals), f32),
            shape(queries.shape, f32),
            shape(keys.shape, f32),
            shape(values.shape, f32),
        ),
        in_specs=[vmem] * 7 + [hbm] * 5,
        out_specs=(hbm,) * 7,
        scratch_shapes=[
            pltpu.VMEM((width, units), f32),
            pltpu.VMEM((width, units), f32),
            pltpu.VMEM((units, width), f32),
            pltpu.VMEM((rows, vals), f32),
            pltpu.VMEM(queries.shape, f32),
            pltpu.VMEM(keys.shape, f32),
            pltpu.VMEM(values.shape, f32),
            pltpu.VMEM((width, units), bf),
            pltpu.VMEM((width, units), bf),
            pltpu.VMEM((units, width), bf),
            pltpu.VMEM(out_w.shape, bf),
            pltpu.VMEM((count, 2, cap, wide), bf),
            pltpu.VMEM((2, cap, wide), bf),
            pltpu.VMEM((4, 2, count, cap, wide), bf),
            pltpu.VMEM((3, slots, units), bf),
            pltpu.VMEM((4, slots, wide), bf),
            pltpu.VMEM((2, slots, wide), bf),
            pltpu.VMEM((slots, wide), bf),
            pltpu.VMEM((slots, wide), bf),
            pltpu.VMEM((slots, wide), bf),
            pltpu.VMEM((count, cap, wide), bf),
            pltpu.VMEM((tokens, wide), f32),
            pltpu.VMEM((4, tokens, wide), bf),
            pltpu.VMEM((count,) + retained.shape, bf),
            pltpu.VMEM((tokens, DV), bf),
            pltpu.VMEM((width, tokens), bf),
            pltpu.VMEM((count, 4, rows // 4, tokens), bf),
            pltpu.VMEM((tokens, tokens), bf),
            pltpu.VMEM((tokens, tokens), bf),
            dma((5,)),
            dma((7,)),
        ]
        + [dma((count,))] * 14
        + [dma((GROUPS,))] * 4
        + [dma((6,))] * 2
        + chain_scratch()
        + chain_scratch(),
        compiler_params=pltpu.CompilerParams(
            collective_id=0, has_side_effects=True, vmem_limit_bytes=62 * 2**20
        ),
        name="layer",
    )(
        place,
        row_weight,
        hidden,
        cotangent,
        queries,
        keys,
        values,
        gate_w,
        up_w,
        down_w,
        out_w,
        retained,
    )


def routing(routes, route_weight, experts_all, tok_local):
    top_count = routes.shape[1]
    capacity = 3 * tok_local * top_count // (2 * experts_all)
    capacity = -(-capacity // 16) * 16
    ids = jnp.arange(experts_all, dtype=jnp.int32)[:, None]
    named = [routes[:, r][None, :] == ids for r in range(top_count)]
    member = sum(m.astype(jnp.float32) for m in named)
    slot_weight = sum(jnp.where(m, route_weight[:, r][None, :], 0.0) for r, m in enumerate(named))
    order = jnp.arange(tok_local, dtype=jnp.int32)
    earlier = (order[:, None] < order[None, :]).astype(jnp.bfloat16)
    rank = jnp.dot(member.astype(jnp.bfloat16), earlier, preferred_element_type=jnp.float32)
    rank = jnp.where(member > 0.0, rank, -1.0).astype(jnp.int32)
    hit = rank[:, None, :] == jnp.arange(capacity, dtype=jnp.int32)[None, :, None]
    row_weight = jnp.sum(jnp.where(hit, slot_weight[:, None, :], 0.0), axis=2, keepdims=True)
    return hit.astype(jnp.bfloat16), row_weight


def local(
    hidden,
    cotangent,
    retained,
    queries,
    key_rows,
    value_rows,
    routes,
    route_weight,
    gate_weight,
    up_weight,
    down_weight,
    out_weight,
):
    experts_all = gate_weight.shape[0] * lax.axis_size("sp")
    assert gate_weight.shape[0] == 1 and queries.shape[1] == DK
    place_rows, row_weight = routing(routes, route_weight, experts_all, hidden.shape[0])
    outs = whole_layer(
        place_rows,
        row_weight,
        hidden,
        cotangent,
        queries,
        key_rows,
        value_rows,
        gate_weight[0],
        up_weight[0],
        down_weight[0],
        out_weight,
        retained,
    )
    order = (4, 5, 3, 6, 0, 1, 2)
    outs = dict(zip(order, publish(*(outs[i] for i in order))))
    gate_grad, up_grad, down_grad, proj_grad = (outs[i] for i in range(4))
    query_gradient, key_gradient, value_gradient = (outs[i] for i in range(4, 7))
    return (
        gate_grad[None],
        up_grad[None],
        down_grad[None],
        proj_grad,
        query_gradient,
        key_gradient,
        value_gradient,
    )


def solution(mesh):
    return jax.shard_map(
        local,
        mesh=mesh,
        in_specs=(
            P("sp", None),
            P("sp", None),
            P("sp", "tp"),
            P("sp", "tp"),
            P("sp", "tp"),
            P("sp", "tp"),
            P("sp", None),
            P("sp", None),
            P("sp", None, "tp"),
            P("sp", None, "tp"),
            P("sp", "tp", None),
            P(None, "tp"),
        ),
        out_specs=(
            P("sp", None, "tp"),
            P("sp", None, "tp"),
            P("sp", "tp", None),
            P("sp", "tp"),
            P("sp", "tp"),
            P("sp", "tp"),
            P("sp", "tp"),
        ),
        check_vma=False,
    )
```

```python
import functools
import math

import jax
import jax.numpy as jnp
from jax import lax
from jax.experimental import pallas as pl
from jax.experimental.pallas import tpu as pltpu
from jax.sharding import PartitionSpec as P

H = 4
DK = 256
DV = 512
GROUPS = 8
LINKS = 4
MESH = pl.DeviceIdType.MESH
ROWS = (((0,), (0,)), ((), ()))
COLS = (((1,), (1,)), ((), ()))


def dot(a, b, dims=(((1,), (0,)), ((), ()))):
    return lax.dot_general(a, b, dims, preferred_element_type=jnp.float32)


class Chain:
    def __init__(self, count, reverse, log_span, own, pair_in, summed, link_in, link_out, out_half,
                 state, sems):
        self.sp, self.tp = lax.axis_index("sp"), lax.axis_index("tp")
        self.y = self.sp % 2
        self.yy = self.y if reverse else 1 - self.y
        self.pairs = count // 2
        z = self.sp // 2
        self.t = self.pairs - 1 - z if reverse else z
        self.next = jnp.where(self.t < self.pairs - 1, self.sp - 2 if reverse else self.sp + 2, self.sp)
        self.decay = jnp.exp(jnp.full((8, 128), log_span, jnp.float32))[0:1, 0:1]
        self.own, self.pair_in, self.summed = own, pair_in, summed
        self.link_in, self.link_out, self.out_half, self.state = link_in, link_out, out_half, state
        self.ps, self.pr, self.ls, self.lr, self.bs, self.br = sems
        self.chunks = link_in.shape[0]
        self.wide = link_in.shape[2]

    def pair(self, src, dst, s, r):
        peer = (jnp.bitwise_xor(self.sp, 1), self.tp)
        return pltpu.make_async_remote_copy(src, dst, s, r, device_id=peer, device_id_type=MESH)

    def link(self, c):
        return pltpu.make_async_remote_copy(
            self.link_out.at[c],
            self.link_in.at[c],
            self.ls.at[c],
            self.lr.at[c],
            device_id=(self.next, self.tp),
            device_id_type=MESH,
        )

    def start(self):
        @pl.when(self.t == 0)
        def _():
            self.link_in[...] = jnp.zeros_like(self.link_in)

        self.one = self.pair(self.own.at[1 - self.y], self.pair_in, self.ps, self.pr)
        self.one.start()

    def fold(self):
        self.one.wait_recv()
        g = self.decay
        mine = jnp.where(self.yy == 0, 1.0, g) * self.own[self.y].astype(jnp.float32)
        theirs = jnp.where(self.yy == 0, g, 1.0) * self.pair_in[...].astype(jnp.float32)
        self.summed[...] = mine + theirs

    def step(self, i):
        if i >= self.pairs:
            return

        @pl.when(self.t == i)
        def _():
            for c in range(self.chunks):
                if i > 0:
                    self.link(c).wait_recv()
                if i < self.pairs - 1:
                    value = self.summed[:, c * self.wide : (c + 1) * self.wide]
                    if i > 0:
                        value = value + self.decay * self.decay * self.link_in[c].astype(jnp.float32)
                    self.link_out[c] = value.astype(jnp.bfloat16)
                    self.link(c).start()

    def finish(self):
        g = self.decay
        for c in range(self.chunks):
            cols = slice(c * self.wide, (c + 1) * self.wide)
            ahead = self.link_in[c].astype(jnp.float32)
            own = self.own[self.y, :, cols].astype(jnp.float32)
            near = self.pair_in[:, cols].astype(jnp.float32)
            mine = jnp.where(self.yy == 0, near + g * ahead, ahead)
            theirs = jnp.where(self.yy == 0, ahead, own + g * ahead)
            self.state[self.y, :, cols] = mine.astype(jnp.bfloat16)
            self.out_half[:, cols] = theirs.astype(jnp.bfloat16)
        self.two = self.pair(self.out_half, self.state.at[self.y], self.bs, self.br)
        self.two.start()

    def wait(self):
        self.pair(self.out_half, self.state.at[1 - self.y], self.bs, self.br).wait_recv()

    def drain(self):
        self.one.wait_send()
        self.two.wait_send()

        @pl.when(self.t < self.pairs - 1)
        def _():
            for c in range(self.chunks):
                self.link(c).wait_send()


def chain_scratch():
    half = DK // 2
    return [
        pltpu.VMEM((2, half, DV), jnp.bfloat16),
        pltpu.VMEM((half, DV), jnp.bfloat16),
        pltpu.VMEM((half, DV), jnp.float32),
        pltpu.VMEM((LINKS, half, DV // LINKS), jnp.bfloat16),
        pltpu.VMEM((LINKS, half, DV // LINKS), jnp.bfloat16),
        pltpu.VMEM((half, DV), jnp.bfloat16),
        pltpu.VMEM((2, half, DV), jnp.bfloat16),
        pltpu.SemaphoreType.DMA,
        pltpu.SemaphoreType.DMA,
        pltpu.SemaphoreType.DMA((LINKS,)),
        pltpu.SemaphoreType.DMA((LINKS,)),
        pltpu.SemaphoreType.DMA,
        pltpu.SemaphoreType.DMA,
    ]


def rates(tokens):
    tp = lax.axis_index("tp")
    logs, scales = [], []
    for h in range(H):
        exponent = -5.0 - h if 2 * h < H else -math.log2(tokens) - (h - H // 2)
        logs.append(math.log1p(-(2.0**exponent)))
        scales.append(math.sqrt(-math.expm1(2.0 * logs[-1])))
    log_gamma, scale = jnp.float32(logs[0]), jnp.float32(scales[0])
    for h in range(1, H):
        log_gamma = jnp.where(tp == h, jnp.float32(logs[h]), log_gamma)
        scale = jnp.where(tp == h, jnp.float32(scales[h]), scale)
    return log_gamma, scale


def positions(shape, axis):
    return lax.broadcasted_iota(jnp.int32, shape, axis).astype(jnp.float32)


def layer_kernel(
    count,
    cap,
    routes_ref,
    weight_ref,
    hid_hbm,
    cot_hbm,
    q_hbm,
    k_hbm,
    v_hbm,
    wg_hbm,
    wu_hbm,
    wd_hbm,
    wo_hbm,
    kept_hbm,
    gg,
    ug,
    dg,
    pg,
    qg,
    kg,
    vg,
    place_ref,
    hid_ref,
    cot_ref,
    q_ref,
    k_ref,
    v_ref,
    wg,
    wu,
    wd,
    wo,
    packed,
    packed2,
    got,
    terms,
    part,
    half,
    kept,
    moving,
    other,
    ret,
    total,
    layer,
    spread,
    mixed_ref,
    flipped,
    blocks,
    near_v,
    near_k,
    load_sem,
    d_s,
    d_r,
    a_s,
    a_r,
    b_s,
    b_r,
    c_s,
    c_r,
    r_s,
    r_r,
    k_s,
    k_r,
    p_s,
    p_r,
    h_s,
    h_r,
    x_s,
    x_r,
    l_s,
    l_r,
    *chain_refs,
):
    sp = lax.axis_index("sp")
    tp = lax.axis_index("tp")
    bf = jnp.bfloat16
    tokens, width = hid_hbm.shape
    wide = width // 4
    per = count // GROUPS
    n = per * cap
    offs = [pl.multiple_of(jnp.bitwise_xor(tp, r) * wide, wide) for r in range(4)]
    cols = [pl.ds(o, wide) for o in offs]

    places = (
        (hid_hbm, hid_ref),
        (cot_hbm, cot_ref),
        (k_hbm, k_ref),
        (v_hbm, v_ref),
        (wg_hbm, wg),
        (wu_hbm, wu),
        (wd_hbm, wd),
        (kept_hbm, spread.at[0]),
        (q_hbm, q_ref),
        (wo_hbm, wo),
    )
    loads = [pltpu.make_async_copy(src, dst, load_sem.at[i]) for i, (src, dst) in enumerate(places)]
    for load in loads:
        load.start()

    def along_sp(m, src, dst, s, r):
        peer = (jnp.bitwise_xor(sp, m), tp)
        return pltpu.make_async_remote_copy(src, dst, s, r, device_id=peer, device_id_type=MESH)

    def along_tp(m, src, dst, s, r):
        peer = (sp, jnp.bitwise_xor(tp, m))
        return pltpu.make_async_remote_copy(src, dst, s, r, device_id=peer, device_id_type=MESH)

    barrier = pltpu.get_barrier_semaphore()
    for m in range(1, count):
        pl.semaphore_signal(
            barrier, inc=1, device_id=(jnp.bitwise_xor(sp, m), tp), device_id_type=MESH
        )
    for m in (1, 2):
        pl.semaphore_signal(
            barrier, inc=1, device_id=(sp, jnp.bitwise_xor(tp, m)), device_id_type=MESH
        )

    sends = []

    def begin(copy):
        copy.start()
        sends.append(copy)
        return copy

    top = routes_ref.shape[0]
    ids = lax.broadcasted_iota(jnp.int32, (count, tokens), 0)
    named = [jnp.bitwise_xor(routes_ref[r : r + 1, :], sp) == ids for r in range(top)]
    member = sum(jnp.where(hit, 1.0, 0.0) for hit in named)
    slot_weight = sum(
        jnp.where(hit, weight_ref[r : r + 1, :], 0.0) for r, hit in enumerate(named)
    )
    earlier = positions((tokens, tokens), 0) < positions((tokens, tokens), 1)
    rank = dot(member.astype(bf), jnp.where(earlier, 1.0, 0.0).astype(bf))
    rank = jnp.where(member > 0.0, rank, -1.0)
    rows_at = positions((cap, tokens), 0)
    scales = {}
    for m in range(count):
        hit = rank[m : m + 1, :] == rows_at
        place_ref[m] = jnp.where(hit, 1.0, 0.0).astype(bf)
        scales[m] = jnp.sum(jnp.where(hit, slot_weight[m : m + 1, :], 0.0), axis=1, keepdims=True)

    def pack(m, r):
        one = place_ref[m]
        rows = dot(one, hid_ref[:, cols[r]]).astype(bf)
        return rows, (scales[m] * dot(one, cot_ref[:, cols[r]])).astype(bf)

    loads[0].wait()
    loads[1].wait()
    arrive = {}
    for m in list(range(2, count)) + [1]:
        packed[m, 0], packed[m, 1] = pack(m, 0)
        if m == 1:
            packed2[0], packed2[1] = pack(1, 2)
        if m == 2:
            pl.semaphore_wait(barrier, count + 1)
        arrive[m] = begin(along_sp(m, packed.at[m], got.at[0, :, m], d_s.at[m], d_r.at[m]))
        if m == 1:
            arrive2 = begin(along_sp(1, packed2, got.at[2, :, 1], d_s.at[0], d_r.at[0]))
    for r in range(4):
        got[r, 0, 0], got[r, 1, 0] = pack(0, r)

    log_gamma, scale = rates(tokens * count)
    set_size = len(chain_refs) // 2
    refs = chain_refs[:set_size]
    chain = Chain(count, False, log_gamma * tokens, *refs[:7], refs[7:])
    prior_ref = refs[6]
    for load in loads[2:4]:
        load.wait()
    faded = k_ref[...] * jnp.exp(log_gamma * (tokens - positions((tokens, DK), 0)))
    refs[0][...] = dot(faded.astype(bf), v_ref[...], ROWS).astype(bf).reshape(refs[0].shape)
    chain.start()

    spreads, seen = {}, set()

    def landed(s):
        if s and s not in seen:
            seen.add(s)
            spreads[s].wait_recv()

    def pass_on(s, bits):
        landed(s)
        for bit in bits:
            to = s | bit
            spreads[to] = begin(along_sp(bit, spread.at[s], spread.at[to], k_s.at[to], k_r.at[to]))

    far = count // 2
    near_bits = [1 << i for i in range(far.bit_length() - 1)][::-1]
    loads[7].wait()
    pass_on(0, near_bits)

    from_pair, from_x, from_diag = {}, {}, {}

    def relay_first(m):
        arrive[m].wait_recv()
        if m > 1:
            from_x[m] = begin(along_tp(2, got.at[0, :, m], got.at[2, :, m], b_s.at[m], b_r.at[m]))
        from_pair[m] = begin(along_tp(1, got.at[0, :, m], got.at[1, :, m], a_s.at[m], a_r.at[m]))

    def relay_second(m):
        if m > 1:
            from_x[m].wait_recv()
        else:
            arrive2.wait_recv()
        from_diag[m] = begin(along_tp(1, got.at[2, :, m], got.at[3, :, m], c_s.at[m], c_r.at[m]))

    def slots(g):
        return range(max(1, g * per), (g + 1) * per)

    def rows_of(a, r, g):
        return got[r, a, g * per : (g + 1) * per].reshape(n, wide)

    halves, across, back = {}, {}, {}

    def expert(g):
        for m in slots(g):
            from_pair[m].wait_recv()
            from_diag[m].wait_recv()
        gate_pre = sum(dot(rows_of(0, r, g), wg[cols[r], :]) for r in range(4))
        up_pre = sum(dot(rows_of(0, r, g), wu[cols[r], :]) for r in range(4))
        unit = sum(dot(rows_of(1, r, g), wd[:, cols[r]], COLS) for r in range(4))
        sigma = jax.nn.sigmoid(gate_pre)
        active = gate_pre * sigma
        span = pl.ds(g * n, n)
        terms[0, span] = (active * up_pre).astype(bf)
        gate_term = (unit * up_pre * sigma * (1.0 + gate_pre * (1.0 - sigma))).astype(bf)
        up_term = (unit * active).astype(bf)
        terms[1, span] = gate_term
        terms[2, span] = up_term
        for at, r in ((2, 1), (3, 3), (0, 0), (1, 2)):
            piece = dot(gate_term, wg[cols[r], :], COLS) + dot(up_term, wu[cols[r], :], COLS)
            part[at, span] = piece.astype(bf)
            if at == 3:
                halves[g] = begin(
                    along_tp(1, part.at[2:4, span], half.at[:, span], h_s.at[g], h_r.at[g])
                )

    def cross(g):
        span = pl.ds(g * n, n)
        halves[g].wait_recv()
        mine = part[1, span].astype(jnp.float32) + half[1, span].astype(jnp.float32)
        moving[span] = mine.astype(bf)
        across[g] = begin(along_tp(2, moving.at[span], other.at[span], x_s.at[g], x_r.at[g]))
        mine = part[0, span].astype(jnp.float32) + half[0, span].astype(jnp.float32)
        kept[span] = mine.astype(bf)

    def give_back(g):
        across[g].wait_recv()
        for m in range(g * per, (g + 1) * per):
            span = pl.ds(m * cap, cap)
            done = (kept[span].astype(jnp.float32) + other[span].astype(jnp.float32)).astype(bf)
            if m == 0:
                ret[0] = done
            else:
                kept[span] = done
                back[m] = begin(along_sp(m, kept.at[span], ret.at[m], r_s.at[m], r_r.at[m]))

    for m in slots(0):
        relay_first(m)
        relay_second(m)
    for load in loads[4:7] + loads[8:]:
        load.wait()
    expert(0)
    turns = [0] + list(range(2, GROUPS))
    for i in range(1, GROUPS - 1):
        for m in slots(turns[i]):
            relay_first(m)
        if i > 1:
            for m in slots(turns[i - 1]):
                relay_second(m)
        if i > 2:
            give_back(turns[i - 3])
        if i == 1:
            cross(0)
        elif i > 2:
            cross(turns[i - 2])
        if i > 1:
            expert(turns[i - 1])
        if i == GROUPS // 2:
            pass_on(0, [far])
    for s in sorted(range(2, far, 2), key=lambda s: bin(s).count("1")):
        low = s & -s
        pass_on(s, [b for b in near_bits if b < low])
    for m in slots(1):
        relay_first(m)
        relay_second(m)
    give_back(turns[-3])
    cross(turns[-2])
    expert(1)
    chain.fold()
    chain.step(0)
    for m in slots(turns[-1]):
        relay_second(m)
    cross(1)
    give_back(turns[-2])
    expert(turns[-1])
    give_back(1)
    pass_on(far, near_bits)
    cross(turns[-1])

    def whole(a, r):
        return got[r, a].reshape(count * cap, wide)

    for r in range(4):
        dg[:, cols[r]] = dot(terms[0], whole(1, r), ROWS)
    give_back(turns[-1])
    chain.step(1)
    total[...] = cot_ref[:, cols[0]].astype(jnp.float32)
    for m in range(count):
        if m:
            back[m].wait_recv()
        total[...] += dot(place_ref[m], ret[m], ROWS)
    layer[0] = total[...].astype(bf)
    one = begin(along_tp(2, layer.at[0], layer.at[2], l_s.at[0], l_r.at[0]))
    two = begin(along_tp(1, layer.at[0], layer.at[1], l_s.at[1], l_r.at[1]))
    for j in range(2, count // 2 - 1):
        chain.step(j)

    step = min(256, wide)
    eye = (positions((step, step), 0) == positions((step, step), 1)).astype(bf)

    def flip(r):
        for c in range(wide // step):
            at = pl.multiple_of(offs[r] + c * step, step)
            flipped[pl.ds(at, step), :] = dot(eye, layer[r, :, c * step : (c + 1) * step], COLS).astype(bf)

    total[...] = dot(layer[0], wo[cols[0], :])
    flip(0)
    two.wait_recv()
    total[...] += dot(layer[1], wo[cols[1], :])
    flip(1)
    faded = (q_ref[...] * jnp.exp(log_gamma * (positions((tokens, DK), 0) + 1.0))).astype(bf)
    for r in range(4):
        gg[cols[r], :] = dot(whole(0, r), terms[1], ROWS)
    for s in sorted(range(far + 2, count, 2), key=lambda s: bin(s).count("1")):
        low = s & -s
        pass_on(s, [b for b in near_bits if b < low])
    chain.step(count // 2 - 1)
    chain.finish()
    one.wait_recv()
    three = begin(along_tp(1, layer.at[2], layer.at[3], l_s.at[2], l_r.at[2]))
    total[...] += dot(layer[2], wo[cols[2], :])
    flip(2)
    three.wait_recv()
    mixed_ref[...] = (total[...] + dot(layer[3], wo[cols[3], :])).astype(bf)
    refs = chain_refs[set_size:]
    ahead = Chain(count, True, log_gamma * tokens, *refs[:7], refs[7:])
    refs[0][...] = dot(faded, mixed_ref[...], ROWS).astype(bf).reshape(refs[0].shape)
    ahead.start()
    flip(3)
    rows = width // count
    share = rows // 4
    for m in range(count):
        at = pl.multiple_of(jnp.bitwise_xor(sp, m) * rows + tp * share, share)
        if m:
            arrive[m] = begin(
                along_sp(m, flipped.at[pl.ds(at, share)], blocks.at[m, 0], p_s.at[m], p_r.at[m])
            )
        else:
            blocks[0, 0] = flipped[pl.ds(at, share)]
    for r in range(4):
        ug[cols[r], :] = dot(whole(0, r), terms[2], ROWS)
    ahead.fold()
    ahead.step(0)
    gap = positions((tokens, tokens), 0) - positions((tokens, tokens), 1)
    fade = jnp.where(gap >= 0, scale * jnp.exp(log_gamma * jnp.maximum(gap, 0.0)), 0.0)
    near_v[...] = (dot(mixed_ref[...], v_ref[...], COLS) * fade).astype(bf)
    near_k[...] = (dot(q_ref[...], k_ref[...], COLS) * fade).astype(bf)
    ahead.step(1)
    lead = scale * jnp.exp(log_gamma * positions((tokens, DK), 0))
    chain.wait()
    prior = prior_ref[...].reshape(DK, DV)
    qg[...] = dot(near_v[...], k_ref[...]) + lead * dot(mixed_ref[...], prior, COLS)
    kg[...] = dot(near_v[...], q_ref[...], ROWS)
    vg[...] = dot(near_k[...], mixed_ref[...], ROWS)
    for m in range(1, count):
        arrive[m].wait_recv()
    over_x = begin(along_tp(2, blocks.at[:, 0], blocks.at[:, 2], l_s.at[3], l_r.at[3]))
    over_pair = begin(along_tp(1, blocks.at[:, 0], blocks.at[:, 1], l_s.at[4], l_r.at[4]))
    for i in range(2, count // 2 - 1):
        ahead.step(i)
    ahead.step(count // 2 - 1)
    ahead.finish()
    over_x.wait_recv()
    diag = begin(along_tp(1, blocks.at[:, 2], blocks.at[:, 3], l_s.at[5], l_r.at[5]))
    over_pair.wait_recv()
    diag.wait_recv()
    for s in spreads:
        landed(s)
    proj = jnp.zeros((rows, spread.shape[2]), jnp.float32)
    for m in range(count):
        proj = proj + dot(blocks[m].reshape(rows, tokens), spread[m])
    proj = proj.reshape(4, share, spread.shape[2])
    for r in range(4):
        at = pl.multiple_of(jnp.bitwise_xor(tp, r) * share, share)
        pg[pl.ds(at, share), :] = proj[r]
    ahead.wait()
    later = refs[6][...].reshape(DK, DV)
    trail = scale * jnp.exp(log_gamma * (tokens - 1.0 - positions((tokens, DV), 0)))
    kg[...] += trail[:, :DK] * dot(v_ref[...], later, COLS)
    vg[...] += trail * dot(k_ref[...], later)
    for copy in sends:
        copy.wait_send()
    chain.drain()
    ahead.drain()


def publish_kernel(count, *refs):
    srcs, dsts, sems = refs[:count], refs[count : 2 * count], refs[-1]
    outs = [pltpu.make_async_copy(srcs[i], dsts[i], sems.at[i]) for i in range(count)]
    for copy in outs:
        copy.start()
    for copy in outs:
        copy.wait()


def publish(*arrays):
    count = len(arrays)
    return pl.pallas_call(
        functools.partial(publish_kernel, count),
        out_shape=tuple(jax.ShapeDtypeStruct(a.shape, a.dtype) for a in arrays),
        in_specs=[pl.BlockSpec(memory_space=pltpu.VMEM)] * count,
        out_specs=(pl.BlockSpec(memory_space=pl.ANY),) * count,
        scratch_shapes=[pltpu.SemaphoreType.DMA((count,))],
        compiler_params=pltpu.CompilerParams(vmem_limit_bytes=16 * 2**20),
        name="publish",
    )(*arrays)


def whole_layer(
    routes, route_weight, hidden, cotangent, queries, keys, values, gate_w, up_w, down_w, out_w, retained
):
    count = lax.axis_size("sp")
    assert lax.axis_size("tp") == 4 and count % GROUPS == 0
    tokens, width = hidden.shape
    cap = 3 * tokens * routes.shape[1] // (2 * count)
    cap = -(-cap // 16) * 16
    units = gate_w.shape[1]
    wide = width // 4
    slots = count * cap
    rows, vals = width // count, retained.shape[1]
    bf, f32 = jnp.bfloat16, jnp.float32
    dma = pltpu.SemaphoreType.DMA
    vmem = pl.BlockSpec(memory_space=pltpu.VMEM)
    hbm = pl.BlockSpec(memory_space=pl.ANY)
    shape = pltpu.VMEM
    return pl.pallas_call(
        functools.partial(layer_kernel, count, cap),
        out_shape=(
            shape((width, units), f32),
            shape((width, units), f32),
            shape((units, width), f32),
            shape((rows, vals), f32),
            shape(queries.shape, f32),
            shape(keys.shape, f32),
            shape(values.shape, f32),
        ),
        in_specs=[vmem] * 2 + [hbm] * 10,
        out_specs=(vmem,) * 7,
        scratch_shapes=[
            pltpu.VMEM((count, cap, tokens), bf),
            pltpu.VMEM((tokens, width), bf),
            pltpu.VMEM((tokens, width), bf),
            pltpu.VMEM(queries.shape, bf),
            pltpu.VMEM(keys.shape, bf),
            pltpu.VMEM(values.shape, bf),
            pltpu.VMEM((width, units), bf),
            pltpu.VMEM((width, units), bf),
            pltpu.VMEM((units, width), bf),
            pltpu.VMEM(out_w.shape, bf),
            pltpu.VMEM((count, 2, cap, wide), bf),
            pltpu.VMEM((2, cap, wide), bf),
            pltpu.VMEM((4, 2, count, cap, wide), bf),
            pltpu.VMEM((3, slots, units), bf),
            pltpu.VMEM((4, slots, wide), bf),
            pltpu.VMEM((2, slots, wide), bf),
            pltpu.VMEM((slots, wide), bf),
            pltpu.VMEM((slots, wide), bf),
            pltpu.VMEM((slots, wide), bf),
            pltpu.VMEM((count, cap, wide), bf),
            pltpu.VMEM((tokens, wide), f32),
            pltpu.VMEM((4, tokens, wide), bf),
            pltpu.VMEM((count,) + retained.shape, bf),
            pltpu.VMEM((tokens, DV), bf),
            pltpu.VMEM((width, tokens), bf),
            pltpu.VMEM((count, 4, rows // 4, tokens), bf),
            pltpu.VMEM((tokens, tokens), bf),
            pltpu.VMEM((tokens, tokens), bf),
            dma((10,)),
        ]
        + [dma((count,))] * 14
        + [dma((GROUPS,))] * 4
        + [dma((6,))] * 2
        + chain_scratch()
        + chain_scratch(),
        compiler_params=pltpu.CompilerParams(
            collective_id=0, has_side_effects=True, vmem_limit_bytes=52 * 2**20
        ),
        name="layer",
    )(
        routes.T,
        route_weight.T,
        hidden,
        cotangent,
        queries,
        keys,
        values,
        gate_w,
        up_w,
        down_w,
        out_w,
        retained,
    )


def local(
    hidden,
    cotangent,
    retained,
    queries,
    key_rows,
    value_rows,
    routes,
    route_weight,
    gate_weight,
    up_weight,
    down_weight,
    out_weight,
):
    assert gate_weight.shape[0] == 1 and queries.shape[1] == DK
    outs = whole_layer(
        routes,
        route_weight,
        hidden,
        cotangent,
        queries,
        key_rows,
        value_rows,
        gate_weight[0],
        up_weight[0],
        down_weight[0],
        out_weight,
        retained,
    )
    order = (4, 5, 3, 6, 0, 1, 2)
    outs = dict(zip(order, publish(*(outs[i] for i in order))))
    gate_grad, up_grad, down_grad, proj_grad = (outs[i] for i in range(4))
    query_gradient, key_gradient, value_gradient = (outs[i] for i in range(4, 7))
    return (
        gate_grad[None],
        up_grad[None],
        down_grad[None],
        proj_grad,
        query_gradient,
        key_gradient,
        value_gradient,
    )


def solution(mesh):
    return jax.shard_map(
        local,
        mesh=mesh,
        in_specs=(
            P("sp", None),
            P("sp", None),
            P("sp", "tp"),
            P("sp", "tp"),
            P("sp", "tp"),
            P("sp", "tp"),
            P("sp", None),
            P("sp", None),
            P("sp", None, "tp"),
            P("sp", None, "tp"),
            P("sp", "tp", None),
            P(None, "tp"),
        ),
        out_specs=(
            P("sp", None, "tp"),
            P("sp", None, "tp"),
            P("sp", "tp", None),
            P("sp", "tp"),
            P("sp", "tp"),
            P("sp", "tp"),
            P("sp", "tp"),
        ),
        check_vma=False,
    )
```
